32 devices in a mesh: grp: 2 (over x), sp: 4 (over z), tp: 4 (over y, core).
Axes of the slice: x: 2, y: 2, z: 4, core: 2. Of those that a mesh axis runs over, the one named last changes fastest.
Arguments:
- stream: bfloat16 [4096, 2560], P(None, ('grp', 'sp')), parts along dimension 1, may hold values from -6 to 6
- norm_gain: float32 [2, 4096], replicated, may hold values from 0.1 to 1.9
- value_weight: bfloat16 [2, 2048, 4096], P(None, 'tp'), may hold values from -0.09375 to 0.09375
- gate_weight: bfloat16 [2, 2048, 4096], P(None, 'tp'), may hold values from -0.09375 to 0.09375
- conv_kernel: float32 [2, 2048, 31], P(None, 'tp')
- conv_bias: float32 [2, 2048], P(None, 'tp'), may hold values from -3 to 3
- channel_gain: float32 [2, 2048], P(None, 'tp'), may hold values from 0.1 to 1.9
- channel_bias: float32 [2, 2048], P(None, 'tp'), may hold values from -3 to 3
- out_weight: bfloat16 [2, 4096, 2048], P(None, 'tp'), may hold values from -0.25 to 0.25
Outputs:
- result: bfloat16 [4096, 2560], P('tp', ('grp', 'sp')), parts along dimension 1
The draws below stay inside these ranges and needn't reach their ends.
There are 2 independent parts, one for each index of `grp`. The reference program is written for one: setup_inputs(seed, part) draws one part's arguments, and reference() takes and returns one part's arrays. A program takes and returns all parts, laid end to end along the dimension named above; an argument that names none is the same for every part. Nothing has to cross between parts.
All inputs are finite; a program needn't handle non-finite values.
Results may differ from the reference program's by a relative error of at most 0.012.
Values may be sent and summed in bfloat16 or wider, within the bound.
A program may use at most 128 MiB of HBM per device.

```python
import math
import jax
import jax.numpy as jnp
from jax import lax

D = 4096
C = 2048
K = 31
LAYERS = 2
TOKENS = 1280


def draw_conv_kernel(key, part):
    normal_key, factor_key = jax.random.split(key)
    samples = jax.random.truncated_normal(normal_key, -4.0, 4.0, (LAYERS, C, K), jnp.float32)
    rising = 10.0 ** (jnp.arange(C, dtype=jnp.float32) / (C - 1))
    jitter = jnp.exp(jax.random.uniform(factor_key, (LAYERS, C, 1), jnp.float32, -0.35, 0.35))
    return samples * rising[None, :, None] * jitter * (0.5 / math.sqrt(K))


def steps_of(stream_key, shape, cuts, smallest, top_value):
    factor_of = 1.0
    for position, blocks in cuts:
        heights = jax.random.uniform(jax.random.fold_in(jax.random.fold_in(stream_key, 6), position), (blocks,), jnp.float32, smallest / len(cuts), top_value / len(cuts))
        factor_of = factor_of * jnp.repeat(jnp.exp(heights), shape[position] // blocks).reshape((-1,) + (1,) * (len(shape) - 1 - position))
    return factor_of


def gaussian(rng, shape, scale, most, pieces=(), kind=jnp.bfloat16):
    loudness = steps_of(rng, shape, pieces, -0.22, 0.18) if pieces else 1.0
    entries = jax.random.normal(rng, shape, jnp.float32) * scale * loudness
    return jnp.minimum(jnp.maximum(entries, -most), most).astype(kind)


def setup_inputs(seed: int = 0, part: int = 0) -> dict:
    keys = jax.random.split(jax.random.key(seed), 10)
    own_keys = jax.random.split(jax.random.fold_in(keys[9], part), 10)
    return {
        "stream": gaussian(own_keys[0], (D, TOKENS), 1.0, 6.0, ((1, 4),)),
        "norm_gain": jnp.clip(1.0 + 0.18 * jax.random.normal(keys[1], (LAYERS, D), jnp.float32), 0.1, 1.9),
        "value_weight": gaussian(keys[2], (LAYERS, C, D), D ** -0.5, 0.09375, ((1, 4),)),
        "gate_weight": gaussian(keys[3], (LAYERS, C, D), D ** -0.5, 0.09375, ((1, 4),)),
        "conv_kernel": draw_conv_kernel(jax.random.fold_in(keys[9], 71), part),
        "conv_bias": gaussian(keys[5], (LAYERS, C), 0.5, 3.0, ((1, 4),), jnp.float32),
        "channel_gain": jnp.clip(1.0 + 0.18 * jax.random.normal(keys[6], (LAYERS, C), jnp.float32), 0.1, 1.9),
        "channel_bias": gaussian(keys[7], (LAYERS, C), 0.5, 3.0, ((1, 4),), jnp.float32),
        "out_weight": gaussian(keys[8], (LAYERS, D, C), (C // 4) ** -0.5, 0.25, ((1, 4),)),
    }


epsilon = 1e-06

def depthwise(signal, kernel):
    length = signal.shape[0]
    padded = jnp.pad(signal, ((K - 1, 0), (0, 0)))
    total = jnp.zeros_like(signal)
    for tap in range(K):
        total = total + padded[tap:tap + length] * kernel[:, tap][None, :]
    return total

def reference(stream, norm_gain, value_weight, gate_weight, conv_kernel, conv_bias, channel_gain, channel_bias, out_weight):
    rows = stream.T
    for layer in range(LAYERS):
        current = rows.astype(jnp.float32)
        scaling = lax.rsqrt(lax.optimization_barrier(jnp.mean(current * current, axis=1, keepdims=True)) + epsilon)
        normed = (current * scaling * norm_gain[layer]).astype(jnp.bfloat16)
        value = jnp.dot(normed, value_weight[layer].T, preferred_element_type=jnp.float32)
        gate_part = jnp.dot(normed, gate_weight[layer].T, preferred_element_type=jnp.float32)
        gated = (value * jax.nn.sigmoid(gate_part)).astype(jnp.bfloat16)
        filtered = depthwise(gated.astype(jnp.float32), conv_kernel[layer]) + conv_bias[layer]
        row_mean = lax.optimization_barrier(jnp.mean(filtered, axis=1, keepdims=True))
        centred = filtered - row_mean
        spread = lax.optimization_barrier(jnp.mean(centred * centred, axis=1, keepdims=True))
        activated = jax.nn.silu(centred * lax.rsqrt(spread + epsilon) * channel_gain[layer] + channel_bias[layer]).astype(jnp.bfloat16)
        branch = jnp.dot(activated, out_weight[layer].T, preferred_element_type=jnp.float32)
        rows = (current + branch).astype(jnp.bfloat16)
    return rows.T
```

```python
import functools

import jax
import jax.numpy as jnp
from jax import lax
from jax.experimental import pallas as pl
from jax.experimental.pallas import tpu as pltpu
from jax.sharding import PartitionSpec as P

K = 31
LAYERS = 2


epsilon = 1e-06


def shifted(value, axis, steps):
    count = lax.axis_size(axis)
    initial, last = (max(0, -steps), min(count, count - steps))
    return lax.ppermute(value, axis, [(source, source + steps) for source in range(initial, last)])


def depthwise(signal, kernel):
    out = lax.conv_general_dilated(
        signal[None],
        kernel[:, None, :],
        (1,),
        [(0, 0)],
        dimension_numbers=("NCW", "OIW", "NCW"),
        feature_group_count=kernel.shape[0],
        precision=lax.Precision.HIGHEST,
    )
    return out[0]


def norm_project(whole, gain, weights):
    scaling = lax.rsqrt(jnp.mean(whole * whole, axis=0, keepdims=True) + epsilon)
    normed = (whole * scaling * gain[:, None]).astype(jnp.bfloat16)
    return jnp.dot(weights, normed, preferred_element_type=jnp.float32)


def local(
    stream,
    norm_gain,
    value_weight,
    gate_weight,
    conv_kernel,
    conv_bias,
    channel_gain,
    channel_bias,
    out_weight,
):
    shard_channels = value_weight.shape[1]
    total_channels = shard_channels * lax.axis_size("tp")
    shard_features = out_weight.shape[1]
    tokens_here = stream.shape[1]
    row_start = lax.axis_index("tp") * shard_features
    whole = stream.astype(jnp.float32)
    current = lax.dynamic_slice_in_dim(whole, row_start, shard_features, 0)
    layer_out = stream
    for layer in range(LAYERS):
        both_weights = jnp.concatenate((value_weight[layer], gate_weight[layer]), axis=0)
        if layer == 0:
            projected = norm_project(whole, norm_gain[layer], both_weights)
        else:
            gathered = lax.all_gather(layer_out, "tp", axis=0, tiled=True).astype(jnp.float32)
            projected = norm_project(gathered, norm_gain[layer], both_weights)
        gated = (projected[:shard_channels] * jax.nn.sigmoid(projected[shard_channels:])).astype(
            jnp.bfloat16
        )
        earlier = shifted(gated[:, tokens_here - (K - 1) :], "sp", 1)
        extended = jnp.concatenate((earlier, gated), axis=1).astype(jnp.float32)
        filtered = depthwise(extended, conv_kernel[layer]) + conv_bias[layer][:, None]
        first_sum, square_sum = lax.psum(
            (
                jnp.sum(filtered, axis=0, keepdims=True),
                jnp.sum(filtered * filtered, axis=0, keepdims=True),
            ),
            "tp",
        )
        row_mean = first_sum / total_channels
        centred = filtered - row_mean
        spread = square_sum / total_channels - row_mean * row_mean
        activated = jax.nn.silu(
            centred * lax.rsqrt(spread + epsilon) * channel_gain[layer][:, None]
            + channel_bias[layer][:, None]
        ).astype(jnp.bfloat16)

        def accumulate(total, piece, start, weights=out_weight[layer]):
            weight_cols = lax.dynamic_slice_in_dim(weights, start, piece.shape[0], 1)
            return total + jnp.dot(weight_cols, piece, preferred_element_type=jnp.float32)

        zero_branch = jnp.zeros((shard_features, tokens_here), jnp.float32)
        branch = accumulate(
            zero_branch, lax.all_gather(activated, "tp", axis=0, tiled=True), jnp.int32(0)
        )
        layer_out = (current + branch).astype(jnp.bfloat16)
        current = layer_out.astype(jnp.float32)
    return layer_out


MESH = pl.DeviceIdType.MESH
LANES = 128
CHUNK = 256
HALO = 32
ROWS = 64
CORES = 2
WEIGHT_PIECES = 4


def dot_nt(left, right):
    return lax.dot_general(
        left, right, (((1,), (1,)), ((), ())), preferred_element_type=jnp.float32
    )


def kernel(
    n_tp,
    n_sp,
    x_ref,
    gain_ref,
    param_ref,
    wv_ref,
    wg_ref,
    ow_ref,
    out_ref,
    wp,
    wo,
    xg,
    ext,
    filt,
    part,
    column,
    halo_out,
    halo_in,
    stat,
    ag,
    sg,
    accp,
    acco,
    res,
    wp_sem,
    wo_sem,
    halo_send,
    halo_recv,
    stat_send,
    stat_recv,
    y_send,
    y_recv,
    f_send,
    f_recv,
):
    tokens, width = x_ref.shape
    chans = wv_ref.shape[1]
    feats = ow_ref.shape[1]
    total_chans = chans * n_tp
    n_y = n_tp // CORES
    piece = width // WEIGHT_PIECES
    padded = part.shape[1]
    me = lax.axis_index("tp")
    sp = lax.axis_index("sp")
    my_y, core = me // CORES, me % CORES
    sibling = my_y * CORES + (1 - core)

    def tp_id(index):
        return {"tp": index}

    barrier = pltpu.get_barrier_semaphore()
    for step in range(1, n_tp):
        pl.semaphore_signal(
            barrier, inc=1, device_id=tp_id(lax.rem(me + step, n_tp)), device_id_type=MESH
        )

    @pl.when(sp > 0)
    def _():
        pl.semaphore_signal(barrier, inc=1, device_id={"sp": sp - 1}, device_id_type=MESH)

    @pl.when(sp < n_sp - 1)
    def _():
        pl.semaphore_signal(barrier, inc=1, device_id={"sp": sp + 1}, device_id_type=MESH)

    def proj_copies(layer, index):
        cols = pl.ds(index * piece, piece)
        return [
            pltpu.make_async_copy(
                ref.at[layer, :, cols], wp.at[layer, half, :, cols], wp_sem.at[layer, index]
            )
            for half, ref in enumerate((wv_ref, wg_ref))
        ]

    def out_copy(layer):
        return pltpu.make_async_copy(ow_ref.at[layer], wo.at[layer], wo_sem.at[layer])

    for layer in range(LAYERS):
        for index in range(WEIGHT_PIECES):
            for copy in proj_copies(layer, index):
                copy.start()
        out_copy(layer).start()

    def prepare(layer, read, first_col, cols, first):
        gains = gain_ref[layer : layer + 1, pl.ds(first_col, cols)]

        @pl.loop(0, tokens // ROWS)
        def _(block):
            rows = pl.ds(pl.multiple_of(block * ROWS, ROWS), ROWS)
            squares = jnp.zeros((ROWS, LANES), jnp.float32)
            if not first:
                squares = part[0, rows, :]
            for lane in range(cols // LANES):
                here = slice(lane * LANES, (lane + 1) * LANES)
                values = read(rows, here).astype(jnp.float32)
                squares = squares + values * values
                xg[rows, here] = (values * gains[:, here]).astype(jnp.bfloat16)
            part[0, rows, :] = squares

    def project(layer, first_col, cols, first):
        for half in range(2):
            held = slice(half * chans, (half + 1) * chans)
            product = dot_nt(xg[:, :cols], wp[layer, half, :, pl.ds(first_col, cols)])
            if first:
                accp[:, held] = product
            else:
                accp[:, held] += product

    pending = []

    def remote(source, target, send, recv, device):
        copy = pltpu.make_async_remote_copy(
            src_ref=source,
            dst_ref=target,
            send_sem=send,
            recv_sem=recv,
            device_id=tp_id(device),
            device_id_type=MESH,
        )
        return copy

    def y_copy(phase, buf, step, chunk, owner):
        target = lax.rem(my_y + step, n_y) * CORES + core
        ref = buf.at[owner, chunk]
        return remote(
            ref, ref, y_send.at[phase, step, chunk], y_recv.at[phase, step, chunk], target
        )

    def f_copy(phase, buf, step, chunk, owner):
        ref = buf.at[owner, chunk]
        return remote(
            ref, ref, f_send.at[phase, step, chunk], f_recv.at[phase, step, chunk], sibling
        )

    def send_own(phase, buf, chunk):
        for step in range(1, n_y):
            copy = y_copy(phase, buf, step, chunk, me)
            copy.start()
            pending.append(copy)
        copy = f_copy(phase, buf, 0, chunk, me)
        copy.start()
        pending.append(copy)

    def gather(phase, buf, chunks, use):
        for chunk in range(chunks):
            use(me, chunk, chunk == 0)
        for chunk in range(chunks):
            f_copy(phase, buf, 0, chunk, sibling).wait_recv()
            use(sibling, chunk, False)
        for step in range(1, n_y):
            origin = lax.rem(my_y + n_y - step, n_y) * CORES
            for chunk in range(chunks):
                y_copy(phase, buf, step, chunk, origin + core).wait_recv()
                copy = f_copy(phase, buf, step, chunk, origin + core)
                copy.start()
                pending.append(copy)
                use(origin + core, chunk, False)
                f_copy(phase, buf, step, chunk, origin + 1 - core).wait_recv()
                use(origin + 1 - core, chunk, False)

    def gate(layer, first_row, count):
        rows = pl.ds(first_row, count)
        scaling = lax.rsqrt(
            jnp.sum(part[0, rows, :], axis=1, keepdims=True) / width + epsilon
        )
        value = accp[rows, :chans] * scaling
        gates = accp[rows, chans:] * scaling
        gated = (value * jax.nn.sigmoid(gates)).astype(jnp.bfloat16)
        widened = gated.astype(jnp.float32)
        for lane in range(chans // LANES):
            ext[lane, pl.ds(first_row + HALO, count), :] = widened[
                :, lane * LANES : (lane + 1) * LANES
            ]
        return gated

    def convolve(layer, blocks):
        @pl.loop(0, chans // LANES)
        def _(lane):
            here = pl.ds(pl.multiple_of(lane * LANES, LANES), LANES)
            bias = jnp.broadcast_to(param_ref[layer, K : K + 1, here], (ROWS, LANES))
            for block in blocks:
                first_row = block * ROWS
                rows = slice(first_row, first_row + ROWS)
                total = bias
                for tap in range(K):
                    start = first_row + HALO - K + 1 + tap
                    window = ext[lane, start : start + ROWS, :]
                    total = total + window * param_ref[layer, tap : tap + 1, here]
                filt[rows, here] = total
                part[0, rows, :] += total
                part[1, rows, :] += total * total

    for layer in range(LAYERS):
        if layer == 0:
            for index in range(WEIGHT_PIECES):
                start = index * piece
                prepare(
                    layer,
                    lambda rows, here, start=start: x_ref[
                        rows, start + here.start : start + here.stop
                    ],
                    start,
                    piece,
                    index == 0,
                )
                for copy in proj_copies(layer, index):
                    copy.wait()
                project(layer, start, piece, index == 0)
            res[...] = x_ref[:, pl.ds(pl.multiple_of(me * feats, LANES), feats)].astype(jnp.float32)
            pl.semaphore_wait(
                barrier,
                n_tp - 1 + jnp.where(sp > 0, 1, 0) + jnp.where(sp < n_sp - 1, 1, 0),
            )
        else:
            for index in range(WEIGHT_PIECES):
                for copy in proj_copies(layer, index):
                    copy.wait()

            def use_stream(owner, chunk, first):
                start = pl.multiple_of(owner * feats + chunk * CHUNK, LANES)
                prepare(
                    layer,
                    lambda rows, here: sg[owner, chunk, rows, here],
                    start,
                    CHUNK,
                    first,
                )
                project(layer, start, CHUNK, first)

            gather(1, sg, feats // CHUNK, use_stream)

        last_rows = tokens - HALO
        halo_out[layer] = gate(layer, last_rows, HALO)
        to_next = pltpu.make_async_remote_copy(
            src_ref=halo_out.at[layer],
            dst_ref=halo_in.at[layer],
            send_sem=halo_send.at[layer],
            recv_sem=halo_recv.at[layer],
            device_id={"sp": lax.rem(sp + 1, n_sp)},
            device_id_type=MESH,
        )

        @pl.when(sp < n_sp - 1)
        def _():
            to_next.start()

        @pl.loop(0, last_rows // HALO)
        def _(block):
            gate(layer, pl.multiple_of(block * HALO, HALO), HALO)

        part[...] = jnp.zeros(part.shape, jnp.float32)
        convolve(layer, range(1, tokens // ROWS))

        @pl.when(sp > 0)
        def _():
            to_next.wait_recv()
            for lane in range(chans // LANES):
                ext[lane, :HALO, :] = halo_in[
                    layer, :, lane * LANES : (lane + 1) * LANES
                ].astype(jnp.float32)

        @pl.when(sp == 0)
        def _():
            ext[:, :HALO, :] = jnp.zeros((chans // LANES, HALO, LANES), jnp.float32)

        convolve(layer, range(1))
        first_row = jnp.sum(jnp.transpose(part[0]), axis=0, keepdims=True)
        square_row = jnp.sum(jnp.transpose(part[1]), axis=0, keepdims=True)
        row_index = lax.broadcasted_iota(jnp.int32, (8, padded), 0)
        stat[layer, me] = jnp.where(row_index == 0, first_row, square_row)
        stat_copies = []
        for step in range(1, n_tp):
            copy = remote(
                stat.at[layer, me],
                stat.at[layer, me],
                stat_send.at[layer, step],
                stat_recv.at[layer, step],
                lax.rem(me + step, n_tp),
            )
            copy.start()
            pending.append(copy)
            stat_copies.append(copy)
        for step in range(1, n_tp):
            origin = lax.rem(me + n_tp - step, n_tp)
            remote(
                stat.at[layer, origin],
                stat.at[layer, origin],
                stat_send.at[layer, step],
                stat_recv.at[layer, step],
                origin,
            ).wait_recv()
        totals = jnp.sum(stat[layer], axis=0) / total_chans
        mean_row = totals[0:1]
        rstd_row = lax.rsqrt(totals[1:2] - mean_row * mean_row + epsilon)
        column[0] = jnp.transpose(jnp.broadcast_to(mean_row, (LANES, padded)))
        column[1] = jnp.transpose(jnp.broadcast_to(rstd_row, (LANES, padded)))

        phase = 0 if layer == 0 else 2
        for chunk in range(chans // CHUNK):

            @pl.loop(0, tokens // ROWS)
            def _(block):
                rows = pl.ds(pl.multiple_of(block * ROWS, ROWS), ROWS)
                for lane in range(CHUNK // LANES):
                    here = slice(chunk * CHUNK + lane * LANES, chunk * CHUNK + (lane + 1) * LANES)
                    values = (filt[rows, here] - column[0, rows, :]) * column[1, rows, :]
                    values = (
                        values * param_ref[layer, K + 1 : K + 2, here]
                        + param_ref[layer, K + 2 : K + 3, here]
                    )
                    ag[layer, me, chunk, rows, lane * LANES : (lane + 1) * LANES] = (
                        jax.nn.silu(values).astype(jnp.bfloat16)
                    )

            send_own(phase, ag.at[layer], chunk)

        out_copy(layer).wait()

        def use_activated(owner, chunk, first):
            start = pl.multiple_of(owner * chans + chunk * CHUNK, LANES)
            product = dot_nt(ag[layer, owner, chunk], wo[layer, :, pl.ds(start, CHUNK)])
            if first:
                acco[...] = res[...] + product
            else:
                acco[...] += product

        gather(phase, ag.at[layer], chans // CHUNK, use_activated)

        if layer < LAYERS - 1:
            for chunk in range(feats // CHUNK):
                here = slice(chunk * CHUNK, (chunk + 1) * CHUNK)
                rounded = acco[:, here].astype(jnp.bfloat16)
                sg[me, chunk] = rounded
                send_own(1, sg, chunk)
                res[:, here] = rounded.astype(jnp.float32)
        else:
            out_ref[...] = acco[...].astype(jnp.bfloat16)

        @pl.when(sp < n_sp - 1)
        def _():
            to_next.wait_send()

    for copy in pending:
        copy.wait_send()


def fused(mesh, stream, norm_gain, value_weight, gate_weight, conv_kernel, conv_bias,
          channel_gain, channel_bias, out_weight):
    n_tp, n_sp = mesh.shape["tp"], mesh.shape["sp"]
    width, tokens = stream.shape
    chans, feats = value_weight.shape[1], out_weight.shape[1]
    fits = (
        n_tp % CORES == 0
        and chans % CHUNK == 0
        and feats % CHUNK == 0
        and width % (WEIGHT_PIECES * CHUNK) == 0
        and tokens % ROWS == 0
        and n_tp <= 8
    )
    if not fits:
        return local(stream, norm_gain, value_weight, gate_weight, conv_kernel, conv_bias,
                     channel_gain, channel_bias, out_weight)
    padded = -(-tokens // LANES) * LANES
    n_y = n_tp // CORES
    n_a, n_f = chans // CHUNK, feats // CHUNK
    most = max(n_a, n_f)
    params = jnp.concatenate(
        (
            jnp.swapaxes(conv_kernel, 1, 2),
            conv_bias[:, None],
            channel_gain[:, None],
            channel_bias[:, None],
        ),
        axis=1,
    )
    f32, bf16 = jnp.float32, jnp.bfloat16
    vmem = pl.BlockSpec(memory_space=pltpu.VMEM)
    anyspace = pl.BlockSpec(memory_space=pl.ANY)
    out = pl.pallas_call(
        functools.partial(kernel, n_tp, n_sp),
        out_shape=jax.ShapeDtypeStruct((tokens, feats), bf16),
        in_specs=[vmem, vmem, vmem, anyspace, anyspace, anyspace],
        out_specs=vmem,
        scratch_shapes=[
            pltpu.VMEM((LAYERS, 2, chans, width), bf16),
            pltpu.VMEM((LAYERS, feats, chans * n_tp), bf16),
            pltpu.VMEM((tokens, width // WEIGHT_PIECES), bf16),
            pltpu.VMEM((chans // LANES, HALO + tokens, LANES), f32),
            pltpu.VMEM((tokens, chans), f32),
            pltpu.VMEM((2, padded, LANES), f32),
            pltpu.VMEM((2, padded, LANES), f32),
            pltpu.VMEM((LAYERS, HALO, chans), bf16),
            pltpu.VMEM((LAYERS, HALO, chans), bf16),
            pltpu.VMEM((LAYERS, n_tp, 8, padded), f32),
            pltpu.VMEM((LAYERS, n_tp, n_a, tokens, CHUNK), bf16),
            pltpu.VMEM((n_tp, n_f, tokens, CHUNK), bf16),
            pltpu.VMEM((tokens, 2 * chans), f32),
            pltpu.VMEM((tokens, feats), f32),
            pltpu.VMEM((tokens, feats), f32),
            pltpu.SemaphoreType.DMA((LAYERS, WEIGHT_PIECES)),
            pltpu.SemaphoreType.DMA((LAYERS,)),
            pltpu.SemaphoreType.DMA((LAYERS,)),
            pltpu.SemaphoreType.DMA((LAYERS,)),
            pltpu.SemaphoreType.DMA((LAYERS, n_tp)),
            pltpu.SemaphoreType.DMA((LAYERS, n_tp)),
            pltpu.SemaphoreType.DMA((3, n_y, most)),
            pltpu.SemaphoreType.DMA((3, n_y, most)),
            pltpu.SemaphoreType.DMA((3, n_y, most)),
            pltpu.SemaphoreType.DMA((3, n_y, most)),
        ],
        compiler_params=pltpu.CompilerParams(
            collective_id=0, has_side_effects=True, vmem_limit_bytes=60 * 1024 * 1024
        ),
    )(stream.T, norm_gain, params, value_weight, gate_weight, out_weight)
    return out.T


def solution(mesh):
    placed = (
        P(None, ("grp", "sp")),
        P(),
        P(None, "tp", None),
        P(None, "tp", None),
        P(None, "tp", None),
        P(None, "tp"),
        P(None, "tp"),
        P(None, "tp"),
        P(None, "tp", None),
    )
    return jax.shard_map(
        functools.partial(fused, mesh), mesh=mesh, in_specs=placed, out_specs=P("tp", ("grp", "sp")), check_vma=False
    )
```

```python
import functools

import jax
import jax.numpy as jnp
from jax import lax
from jax.experimental import pallas as pl
from jax.experimental.pallas import tpu as pltpu
from jax.sharding import PartitionSpec as P

K = 31
LAYERS = 2


epsilon = 1e-06


def shifted(value, axis, steps):
    count = lax.axis_size(axis)
    initial, last = (max(0, -steps), min(count, count - steps))
    return lax.ppermute(value, axis, [(source, source + steps) for source in range(initial, last)])


def depthwise(signal, kernel):
    out = lax.conv_general_dilated(
        signal[None],
        kernel[:, None, :],
        (1,),
        [(0, 0)],
        dimension_numbers=("NCW", "OIW", "NCW"),
        feature_group_count=kernel.shape[0],
        precision=lax.Precision.HIGHEST,
    )
    return out[0]


def norm_project(whole, gain, weights):
    scaling = lax.rsqrt(jnp.mean(whole * whole, axis=0, keepdims=True) + epsilon)
    normed = (whole * scaling * gain[:, None]).astype(jnp.bfloat16)
    return jnp.dot(weights, normed, preferred_element_type=jnp.float32)


def local(
    stream,
    norm_gain,
    value_weight,
    gate_weight,
    conv_kernel,
    conv_bias,
    channel_gain,
    channel_bias,
    out_weight,
):
    shard_channels = value_weight.shape[1]
    total_channels = shard_channels * lax.axis_size("tp")
    shard_features = out_weight.shape[1]
    tokens_here = stream.shape[1]
    row_start = lax.axis_index("tp") * shard_features
    whole = stream.astype(jnp.float32)
    current = lax.dynamic_slice_in_dim(whole, row_start, shard_features, 0)
    layer_out = stream
    for layer in range(LAYERS):
        both_weights = jnp.concatenate((value_weight[layer], gate_weight[layer]), axis=0)
        if layer == 0:
            projected = norm_project(whole, norm_gain[layer], both_weights)
        else:
            gathered = lax.all_gather(layer_out, "tp", axis=0, tiled=True).astype(jnp.float32)
            projected = norm_project(gathered, norm_gain[layer], both_weights)
        gated = (projected[:shard_channels] * jax.nn.sigmoid(projected[shard_channels:])).astype(
            jnp.bfloat16
        )
        earlier = shifted(gated[:, tokens_here - (K - 1) :], "sp", 1)
        extended = jnp.concatenate((earlier, gated), axis=1).astype(jnp.float32)
        filtered = depthwise(extended, conv_kernel[layer]) + conv_bias[layer][:, None]
        first_sum, square_sum = lax.psum(
            (
                jnp.sum(filtered, axis=0, keepdims=True),
                jnp.sum(filtered * filtered, axis=0, keepdims=True),
            ),
            "tp",
        )
        row_mean = first_sum / total_channels
        centred = filtered - row_mean
        spread = square_sum / total_channels - row_mean * row_mean
        activated = jax.nn.silu(
            centred * lax.rsqrt(spread + epsilon) * channel_gain[layer][:, None]
            + channel_bias[layer][:, None]
        ).astype(jnp.bfloat16)

        def accumulate(total, piece, start, weights=out_weight[layer]):
            weight_cols = lax.dynamic_slice_in_dim(weights, start, piece.shape[0], 1)
            return total + jnp.dot(weight_cols, piece, preferred_element_type=jnp.float32)

        zero_branch = jnp.zeros((shard_features, tokens_here), jnp.float32)
        branch = accumulate(
            zero_branch, lax.all_gather(activated, "tp", axis=0, tiled=True), jnp.int32(0)
        )
        layer_out = (current + branch).astype(jnp.bfloat16)
        current = layer_out.astype(jnp.float32)
    return layer_out


MESH = pl.DeviceIdType.MESH
LANES = 128
CHUNK = 256
HALO = 32
ROWS = 64
CORES = 2
WEIGHT_PIECES = 4


def dot_nt(left, right):
    return lax.dot_general(
        left, right, (((1,), (1,)), ((), ())), preferred_element_type=jnp.float32
    )


def kernel(
    n_tp,
    n_sp,
    x_ref,
    gain_ref,
    taps_ref,
    bias_ref,
    chan_gain_ref,
    chan_bias_ref,
    wv_ref,
    wg_ref,
    ow_ref,
    out_ref,
    wp,
    wo,
    xg,
    ext,
    filt,
    taps,
    norm_squares,
    part,
    column,
    halo_out,
    halo_in,
    stat,
    ag,
    sg,
    accp,
    acco,
    res,
    wp_sem,
    wo_sem,
    halo_send,
    halo_recv,
    stat_send,
    stat_recv,
    y_send,
    y_recv,
    f_send,
    f_recv,
):
    tokens, width = x_ref.shape
    chans = wv_ref.shape[1]
    feats = ow_ref.shape[1]
    total_chans = chans * n_tp
    n_y = n_tp // CORES
    piece = width // WEIGHT_PIECES
    padded = part.shape[2]
    split = (tokens // 2 - HALO) // HALO * HALO
    spans = (
        ((split, tokens), (0, split)),
        ((split + HALO, tokens), (0, split + HALO)),
    )
    me = lax.axis_index("tp")
    sp = lax.axis_index("sp")
    my_y, core = me // CORES, me % CORES
    sibling = my_y * CORES + (1 - core)

    def tp_id(index):
        return {"tp": index}

    barrier = pltpu.get_barrier_semaphore()
    for step in range(1, n_tp):
        pl.semaphore_signal(
            barrier, inc=1, device_id=tp_id(lax.rem(me + step, n_tp)), device_id_type=MESH
        )

    @pl.when(sp > 0)
    def _():
        pl.semaphore_signal(barrier, inc=1, device_id={"sp": sp - 1}, device_id_type=MESH)

    @pl.when(sp < n_sp - 1)
    def _():
        pl.semaphore_signal(barrier, inc=1, device_id={"sp": sp + 1}, device_id_type=MESH)

    def proj_copies(layer, index):
        cols = pl.ds(index * piece, piece)
        return [
            pltpu.make_async_copy(
                ref.at[layer, :, cols], wp.at[layer, half, :, cols], wp_sem.at[layer, index]
            )
            for half, ref in enumerate((wv_ref, wg_ref))
        ]

    def out_copy(layer):
        return pltpu.make_async_copy(ow_ref.at[layer], wo.at[layer], wo_sem.at[layer])

    for layer in range(LAYERS):
        for index in range(WEIGHT_PIECES):
            for copy in proj_copies(layer, index):
                copy.start()
        out_copy(layer).start()

    for layer in range(LAYERS):
        taps[layer] = jnp.transpose(taps_ref[layer])

    def prepare(layer, read, first_col, cols, span, at, first):
        gains = gain_ref[layer : layer + 1, pl.ds(first_col, cols)]

        @pl.loop(0, (span[1] - span[0]) // ROWS)
        def _(block):
            rows = pl.ds(pl.multiple_of(span[0] + block * ROWS, HALO), ROWS)
            squares = jnp.zeros((ROWS, LANES), jnp.float32)
            if not first:
                squares = norm_squares[rows, :]
            for lane in range(cols // LANES):
                here = slice(lane * LANES, (lane + 1) * LANES)
                values = read(rows, here).astype(jnp.float32)
                squares = squares + values * values
                xg[rows, at + here.start : at + here.stop] = (values * gains[:, here]).astype(
                    jnp.bfloat16
                )
            norm_squares[rows, :] = squares

    def project(layer, first_col, cols, span, first):
        rows = slice(*span)
        for half in range(2):
            held = slice(half * chans, (half + 1) * chans)
            product = dot_nt(xg[rows, :cols], wp[layer, half, :, pl.ds(first_col, cols)])
            if first:
                accp[rows, held] = product
            else:
                accp[rows, held] += product

    pending = []

    def remote(source, target, send, recv, device):
        copy = pltpu.make_async_remote_copy(
            src_ref=source,
            dst_ref=target,
            send_sem=send,
            recv_sem=recv,
            device_id=tp_id(device),
            device_id_type=MESH,
        )
        return copy

    def y_copy(phase, buf, step, chunk, owner, rows):
        target = lax.rem(my_y + step, n_y) * CORES + core
        ref = buf.at[owner, chunk, rows]
        return remote(
            ref, ref, y_send.at[phase, step, chunk], y_recv.at[phase, step, chunk], target
        )

    def f_copy(phase, buf, step, chunk, owner, rows):
        ref = buf.at[owner, chunk, rows]
        return remote(
            ref, ref, f_send.at[phase, step, chunk], f_recv.at[phase, step, chunk], sibling
        )

    def send_own(phase, buf, chunk, span):
        rows = pl.ds(span[0], span[1] - span[0])
        for step in range(1, n_y):
            copy = y_copy(phase, buf, step, chunk, me, rows)
            copy.start()
            pending.append(copy)
        copy = f_copy(phase, buf, 0, chunk, me, rows)
        copy.start()
        pending.append(copy)

    def near(phase, buf, chunks, span, use):
        rows = pl.ds(span[0], span[1] - span[0])
        use(me, range(chunks), span, True)
        for chunk in range(chunks):
            f_copy(phase, buf, 0, chunk, sibling, rows).wait_recv()
        use(sibling, range(chunks), span, False)

    def far(phase, buf, chunks, span, use):
        rows = pl.ds(span[0], span[1] - span[0])
        for step in range(1, n_y):
            origin = lax.rem(my_y + n_y - step, n_y) * CORES
            for chunk in range(chunks):
                y_copy(phase, buf, step, chunk, origin + core, rows).wait_recv()
                copy = f_copy(phase, buf, step, chunk, origin + core, rows)
                copy.start()
                pending.append(copy)
                use(origin + core, (chunk,), span, False)
                f_copy(phase, buf, step, chunk, origin + 1 - core, rows).wait_recv()
                use(origin + 1 - core, (chunk,), span, False)

    def gate(first_row, count):
        rows = pl.ds(first_row, count)
        scaling = lax.rsqrt(
            jnp.sum(norm_squares[rows, :], axis=1, keepdims=True) / width + epsilon
        )
        value = accp[rows, :chans] * scaling
        gates = accp[rows, chans:] * scaling
        gated = (value * jax.nn.sigmoid(gates)).astype(jnp.bfloat16)
        widened = gated.astype(jnp.float32)
        for lane in range(chans // LANES):
            ext[lane, pl.ds(first_row + HALO, count), :] = widened[
                :, lane * LANES : (lane + 1) * LANES
            ]
        return gated

    def gate_rows(start, stop):
        @pl.loop(0, (stop - start) // HALO)
        def _(block):
            gate(pl.multiple_of(start + block * HALO, HALO), HALO)

    def halo_copy(layer):
        return pltpu.make_async_remote_copy(
            src_ref=halo_out.at[layer],
            dst_ref=halo_in.at[layer],
            send_sem=halo_send.at[layer],
            recv_sem=halo_recv.at[layer],
            device_id={"sp": lax.rem(sp + 1, n_sp)},
            device_id_type=MESH,
        )

    def send_halo(layer):
        halo_out[layer] = gate(tokens - HALO, HALO)

        @pl.when(sp < n_sp - 1)
        def _():
            halo_copy(layer).start()

    def receive_halo(layer):
        @pl.when(sp > 0)
        def _():
            halo_copy(layer).wait_recv()
            for lane in range(chans // LANES):
                ext[lane, :HALO, :] = halo_in[
                    layer, :, lane * LANES : (lane + 1) * LANES
                ].astype(jnp.float32)

        @pl.when(sp == 0)
        def _():
            ext[:, :HALO, :] = jnp.zeros((chans // LANES, HALO, LANES), jnp.float32)

    def convolve(layer, half, start, stop):
        base = spans[layer][half][0]
        blocks = []
        while start < stop:
            count = min(ROWS, stop - start)
            blocks.append((start, count))
            start += count

        @pl.loop(0, chans // LANES)
        def _(lane):
            here = pl.ds(pl.multiple_of(lane * LANES, LANES), LANES)
            bias = bias_ref[layer : layer + 1, here]
            for first_row, count in blocks:
                rows = slice(first_row, first_row + count)
                total = jnp.broadcast_to(bias, (count, LANES))
                for tap in range(K):
                    begin = first_row + HALO - K + 1 + tap
                    window = ext[lane, begin : begin + count, :]
                    total = total + window * taps[layer, tap : tap + 1, here]
                filt[rows, here] = total
                inner = slice(first_row - base, first_row - base + count)
                part[half, 0, inner, :] += total
                part[half, 1, inner, :] += total * total

    def stat_copy(layer, half, step, owner, target):
        ref = stat.at[layer, half, owner]
        index = layer * 2 + half
        return remote(ref, ref, stat_send.at[index, step], stat_recv.at[index, step], target)

    def send_stats(layer, half):
        first_row = jnp.sum(jnp.transpose(part[half, 0]), axis=0, keepdims=True)
        square_row = jnp.sum(jnp.transpose(part[half, 1]), axis=0, keepdims=True)
        row_index = lax.broadcasted_iota(jnp.int32, (8, padded), 0)
        stat[layer, half, me] = jnp.where(row_index == 0, first_row, square_row)
        for step in range(1, n_tp):
            copy = stat_copy(layer, half, step, me, lax.rem(me + step, n_tp))
            copy.start()
            pending.append(copy)

    def activate(layer, half, phase):
        for step in range(1, n_tp):
            origin = lax.rem(me + n_tp - step, n_tp)
            stat_copy(layer, half, step, origin, origin).wait_recv()
        totals = jnp.sum(stat[layer, half], axis=0) / total_chans
        mean_row = totals[0:1]
        rstd_row = lax.rsqrt(totals[1:2] - mean_row * mean_row + epsilon)
        column[0] = jnp.transpose(jnp.broadcast_to(mean_row, (LANES, padded)))
        column[1] = jnp.transpose(jnp.broadcast_to(rstd_row, (LANES, padded)))
        start, stop = spans[layer][half]
        for chunk in range(chans // CHUNK):

            @pl.loop(0, (stop - start) // HALO)
            def _(block):
                inner = pl.ds(pl.multiple_of(block * HALO, HALO), HALO)
                rows = pl.ds(pl.multiple_of(start + block * HALO, HALO), HALO)
                for lane in range(CHUNK // LANES):
                    here = slice(chunk * CHUNK + lane * LANES, chunk * CHUNK + (lane + 1) * LANES)
                    values = (filt[rows, here] - column[0, inner, :]) * column[1, inner, :]
                    values = (
                        values * chan_gain_ref[layer : layer + 1, here]
                        + chan_bias_ref[layer : layer + 1, here]
                    )
                    ag[layer, me, chunk, rows, lane * LANES : (lane + 1) * LANES] = (
                        jax.nn.silu(values).astype(jnp.bfloat16)
                    )

            send_own(phase, ag.at[layer], chunk, (start, stop))

    def use_activated(layer):
        def use(owner, chunks, span, first):
            rows = slice(*span)
            total = res[rows, :] if first else acco[rows, :]
            for chunk in chunks:
                start = pl.multiple_of(owner * chans + chunk * CHUNK, LANES)
                total = total + dot_nt(
                    ag[layer, owner, chunk, rows, :], wo[layer, :, pl.ds(start, CHUNK)]
                )
            acco[rows, :] = total

        return use

    def use_stream(owner, chunks, span, first):
        start = pl.multiple_of(owner * feats + chunks[0] * CHUNK, LANES)
        for chunk in chunks:
            prepare(
                1,
                lambda rows, here: sg[owner, chunk, rows, here],
                pl.multiple_of(owner * feats + chunk * CHUNK, LANES),
                CHUNK,
                span,
                (chunk - chunks[0]) * CHUNK,
                first and chunk == 0,
            )
        project(1, start, len(chunks) * CHUNK, span, first)

    n_a, n_f = chans // CHUNK, feats // CHUNK
    part[...] = jnp.zeros(part.shape, jnp.float32)
    for index in range(WEIGHT_PIECES):
        start = index * piece
        prepare(
            0,
            lambda rows, here: x_ref[rows, start + here.start : start + here.stop],
            start,
            piece,
            (0, tokens),
            0,
            index == 0,
        )
        for copy in proj_copies(0, index):
            copy.wait()
        project(0, start, piece, (0, tokens), index == 0)
    res[...] = x_ref[:, pl.ds(pl.multiple_of(me * feats, LANES), feats)].astype(jnp.float32)
    pl.semaphore_wait(
        barrier,
        n_tp - 1 + jnp.where(sp > 0, 1, 0) + jnp.where(sp < n_sp - 1, 1, 0),
    )
    late, early = spans[0]
    send_halo(0)
    gate_rows(0, tokens - HALO)
    convolve(0, 0, *late)
    send_stats(0, 0)
    convolve(0, 1, ROWS, early[1])
    receive_halo(0)
    convolve(0, 1, 0, ROWS)
    send_stats(0, 1)
    activate(0, 0, 0)
    activate(0, 1, 1)
    out_copy(0).wait()
    for half, span in enumerate(spans[0]):
        near(half, ag.at[0], n_a, span, use_activated(0))
        far(half, ag.at[0], n_a, span, use_activated(0))
        rows = slice(*span)
        for chunk in range(n_f):
            here = slice(chunk * CHUNK, (chunk + 1) * CHUNK)
            rounded = acco[rows, here].astype(jnp.bfloat16)
            sg[me, chunk, rows, :] = rounded
            send_own(2 + half, sg, chunk, span)
            res[rows, here] = rounded.astype(jnp.float32)
    part[...] = jnp.zeros(part.shape, jnp.float32)
    for index in range(WEIGHT_PIECES):
        for copy in proj_copies(1, index):
            copy.wait()
    near(2, sg, n_f, late, use_stream)
    far(2, sg, n_f, late, use_stream)
    send_halo(1)
    gate_rows(split, tokens - HALO)
    convolve(1, 0, *spans[1][0])
    send_stats(1, 0)
    near(3, sg, n_f, early, use_stream)
    activate(1, 0, 4)
    far(3, sg, n_f, early, use_stream)
    gate_rows(0, split)
    convolve(1, 1, HALO, spans[1][1][1])
    receive_halo(1)
    convolve(1, 1, 0, HALO)
    send_stats(1, 1)
    out_copy(1).wait()
    near(4, ag.at[1], n_a, spans[1][0], use_activated(1))
    activate(1, 1, 5)
    far(4, ag.at[1], n_a, spans[1][0], use_activated(1))
    near(5, ag.at[1], n_a, spans[1][1], use_activated(1))
    far(5, ag.at[1], n_a, spans[1][1], use_activated(1))
    out_ref[...] = acco[...].astype(jnp.bfloat16)

    @pl.when(sp < n_sp - 1)
    def _():
        for layer in range(LAYERS):
            halo_copy(layer).wait_send()

    for copy in pending:
        copy.wait_send()


def fused(mesh, stream, norm_gain, value_weight, gate_weight, conv_kernel, conv_bias,
          channel_gain, channel_bias, out_weight):
    n_tp, n_sp = mesh.shape["tp"], mesh.shape["sp"]
    width, tokens = stream.shape
    chans, feats = value_weight.shape[1], out_weight.shape[1]
    fits = (
        n_tp % CORES == 0
        and chans % CHUNK == 0
        and feats % CHUNK == 0
        and width % (WEIGHT_PIECES * CHUNK) == 0
        and tokens % ROWS == 0
        and (tokens // 2 - HALO) // HALO * HALO % ROWS == 0
        and tokens >= 4 * ROWS
        and LAYERS == 2
        and n_tp <= 8
    )
    if not fits:
        return local(stream, norm_gain, value_weight, gate_weight, conv_kernel, conv_bias,
                     channel_gain, channel_bias, out_weight)
    split = (tokens // 2 - HALO) // HALO * HALO
    padded = -(-(tokens - split) // LANES) * LANES
    n_y = n_tp // CORES
    n_a, n_f = chans // CHUNK, feats // CHUNK
    most = max(n_a, n_f)
    f32, bf16 = jnp.float32, jnp.bfloat16
    vmem = pl.BlockSpec(memory_space=pltpu.VMEM)
    anyspace = pl.BlockSpec(memory_space=pl.ANY)
    out = pl.pallas_call(
        functools.partial(kernel, n_tp, n_sp),
        out_shape=jax.ShapeDtypeStruct((tokens, feats), bf16),
        in_specs=[vmem] * 6 + [anyspace, anyspace, anyspace],
        out_specs=vmem,
        scratch_shapes=[
            pltpu.VMEM((LAYERS, 2, chans, width), bf16),
            pltpu.VMEM((LAYERS, feats, chans * n_tp), bf16),
            pltpu.VMEM((tokens, max(width // WEIGHT_PIECES, feats)), bf16),
            pltpu.VMEM((chans // LANES, HALO + tokens, LANES), f32),
            pltpu.VMEM((tokens, chans), f32),
            pltpu.VMEM((LAYERS, K, chans), f32),
            pltpu.VMEM((tokens, LANES), f32),
            pltpu.VMEM((2, 2, padded, LANES), f32),
            pltpu.VMEM((2, padded, LANES), f32),
            pltpu.VMEM((LAYERS, HALO, chans), bf16),
            pltpu.VMEM((LAYERS, HALO, chans), bf16),
            pltpu.VMEM((LAYERS, 2, n_tp, 8, padded), f32),
            pltpu.VMEM((LAYERS, n_tp, n_a, tokens, CHUNK), bf16),
            pltpu.VMEM((n_tp, n_f, tokens, CHUNK), bf16),
            pltpu.VMEM((tokens, 2 * chans), f32),
            pltpu.VMEM((tokens, feats), f32),
            pltpu.VMEM((tokens, feats), f32),
            pltpu.SemaphoreType.DMA((LAYERS, WEIGHT_PIECES)),
            pltpu.SemaphoreType.DMA((LAYERS,)),
            pltpu.SemaphoreType.DMA((LAYERS,)),
            pltpu.SemaphoreType.DMA((LAYERS,)),
            pltpu.SemaphoreType.DMA((LAYERS * 2, n_tp)),
            pltpu.SemaphoreType.DMA((LAYERS * 2, n_tp)),
            pltpu.SemaphoreType.DMA((6, n_y, most)),
            pltpu.SemaphoreType.DMA((6, n_y, most)),
            pltpu.SemaphoreType.DMA((6, n_y, most)),
            pltpu.SemaphoreType.DMA((6, n_y, most)),
        ],
        compiler_params=pltpu.CompilerParams(
            collective_id=0, has_side_effects=True, vmem_limit_bytes=60 * 1024 * 1024
        ),
    )(stream.T, norm_gain, conv_kernel, conv_bias, channel_gain, channel_bias,
       value_weight, gate_weight, out_weight)
    return out.T


def solution(mesh):
    placed = (
        P(None, ("grp", "sp")),
        P(),
        P(None, "tp", None),
        P(None, "tp", None),
        P(None, "tp", None),
        P(None, "tp"),
        P(None, "tp"),
        P(None, "tp"),
        P(None, "tp", None),
    )
    return jax.shard_map(
        functools.partial(fused, mesh), mesh=mesh, in_specs=placed, out_specs=P("tp", ("grp", "sp")), check_vma=False
    )
```

```python
import functools

import jax
import jax.numpy as jnp
from jax import lax
from jax.experimental import pallas as pl
from jax.experimental.pallas import tpu as pltpu
from jax.sharding import PartitionSpec as P

K = 31
LAYERS = 2


epsilon = 1e-06


def shifted(value, axis, steps):
    count = lax.axis_size(axis)
    initial, last = (max(0, -steps), min(count, count - steps))
    return lax.ppermute(value, axis, [(source, source + steps) for source in range(initial, last)])


def depthwise(signal, kernel):
    out = lax.conv_general_dilated(
        signal[None],
        kernel[:, None, :],
        (1,),
        [(0, 0)],
        dimension_numbers=("NCW", "OIW", "NCW"),
        feature_group_count=kernel.shape[0],
        precision=lax.Precision.HIGHEST,
    )
    return out[0]


def norm_project(whole, gain, weights):
    scaling = lax.rsqrt(jnp.mean(whole * whole, axis=0, keepdims=True) + epsilon)
    normed = (whole * scaling * gain[:, None]).astype(jnp.bfloat16)
    return jnp.dot(weights, normed, preferred_element_type=jnp.float32)


def local(
    stream,
    norm_gain,
    value_weight,
    gate_weight,
    conv_kernel,
    conv_bias,
    channel_gain,
    channel_bias,
    out_weight,
):
    shard_channels = value_weight.shape[1]
    total_channels = shard_channels * lax.axis_size("tp")
    shard_features = out_weight.shape[1]
    tokens_here = stream.shape[1]
    row_start = lax.axis_index("tp") * shard_features
    whole = stream.astype(jnp.float32)
    current = lax.dynamic_slice_in_dim(whole, row_start, shard_features, 0)
    layer_out = stream
    for layer in range(LAYERS):
        both_weights = jnp.concatenate((value_weight[layer], gate_weight[layer]), axis=0)
        if layer == 0:
            projected = norm_project(whole, norm_gain[layer], both_weights)
        else:
            gathered = lax.all_gather(layer_out, "tp", axis=0, tiled=True).astype(jnp.float32)
            projected = norm_project(gathered, norm_gain[layer], both_weights)
        gated = (projected[:shard_channels] * jax.nn.sigmoid(projected[shard_channels:])).astype(
            jnp.bfloat16
        )
        earlier = shifted(gated[:, tokens_here - (K - 1) :], "sp", 1)
        extended = jnp.concatenate((earlier, gated), axis=1).astype(jnp.float32)
        filtered = depthwise(extended, conv_kernel[layer]) + conv_bias[layer][:, None]
        first_sum, square_sum = lax.psum(
            (
                jnp.sum(filtered, axis=0, keepdims=True),
                jnp.sum(filtered * filtered, axis=0, keepdims=True),
            ),
            "tp",
        )
        row_mean = first_sum / total_channels
        centred = filtered - row_mean
        spread = square_sum / total_channels - row_mean * row_mean
        activated = jax.nn.silu(
            centred * lax.rsqrt(spread + epsilon) * channel_gain[layer][:, None]
            + channel_bias[layer][:, None]
        ).astype(jnp.bfloat16)

        def accumulate(total, piece, start, weights=out_weight[layer]):
            weight_cols = lax.dynamic_slice_in_dim(weights, start, piece.shape[0], 1)
            return total + jnp.dot(weight_cols, piece, preferred_element_type=jnp.float32)

        zero_branch = jnp.zeros((shard_features, tokens_here), jnp.float32)
        branch = accumulate(
            zero_branch, lax.all_gather(activated, "tp", axis=0, tiled=True), jnp.int32(0)
        )
        layer_out = (current + branch).astype(jnp.bfloat16)
        current = layer_out.astype(jnp.float32)
    return layer_out


MESH = pl.DeviceIdType.MESH
LANES = 128
CHUNK = 256
HALO = 32
ROWS = 64
CORES = 2
WEIGHT_PIECES = 4


def dot_nt(left, right):
    return lax.dot_general(
        left, right, (((1,), (1,)), ((), ())), preferred_element_type=jnp.float32
    )


def kernel(
    n_tp,
    n_sp,
    x_ref,
    gain_ref,
    taps_ref,
    bias_ref,
    chan_gain_ref,
    chan_bias_ref,
    wv_ref,
    wg_ref,
    ow_ref,
    out_ref,
    wp,
    wo,
    xg,
    ext,
    filt,
    taps,
    norm_squares,
    part,
    column,
    halo_out,
    halo_in,
    stat,
    ag,
    sg,
    accp,
    acco,
    res,
    wp_sem,
    wo_sem,
    halo_send,
    halo_recv,
    stat_send,
    stat_recv,
    y_send,
    y_recv,
    f_send,
    f_recv,
):
    tokens, width = x_ref.shape
    chans = wv_ref.shape[1]
    feats = ow_ref.shape[1]
    total_chans = chans * n_tp
    n_y = n_tp // CORES
    piece = width // WEIGHT_PIECES
    padded = part.shape[2]
    split = (tokens // 2 - HALO) // HALO * HALO
    spans = (
        ((split, tokens), (0, split)),
        ((split + HALO, tokens), (0, split + HALO)),
    )
    me = lax.axis_index("tp")
    sp = lax.axis_index("sp")
    my_y, core = me // CORES, me % CORES
    sibling = my_y * CORES + (1 - core)

    def tp_id(index):
        return {"tp": index}

    barrier = pltpu.get_barrier_semaphore()
    for step in range(1, n_tp):
        pl.semaphore_signal(
            barrier, inc=1, device_id=tp_id(lax.rem(me + step, n_tp)), device_id_type=MESH
        )

    @pl.when(sp > 0)
    def _():
        pl.semaphore_signal(barrier, inc=1, device_id={"sp": sp - 1}, device_id_type=MESH)

    @pl.when(sp < n_sp - 1)
    def _():
        pl.semaphore_signal(barrier, inc=1, device_id={"sp": sp + 1}, device_id_type=MESH)

    def proj_copies(layer, index):
        cols = pl.ds(index * piece, piece)
        return [
            pltpu.make_async_copy(
                ref.at[layer, :, cols], wp.at[layer, half, :, cols], wp_sem.at[layer, index]
            )
            for half, ref in enumerate((wv_ref, wg_ref))
        ]

    def out_copy(layer):
        return pltpu.make_async_copy(ow_ref.at[layer], wo.at[layer], wo_sem.at[layer])

    for layer in range(LAYERS):
        for index in range(WEIGHT_PIECES):
            for copy in proj_copies(layer, index):
                copy.start()
        out_copy(layer).start()

    for layer in range(LAYERS):
        taps[layer] = taps_ref[:, layer, :]

    def prepare(layer, read, first_col, cols, span, at, first):
        gains = gain_ref[layer : layer + 1, pl.ds(first_col, cols)]

        @pl.loop(0, (span[1] - span[0]) // ROWS)
        def _(block):
            rows = pl.ds(pl.multiple_of(span[0] + block * ROWS, HALO), ROWS)
            squares = jnp.zeros((ROWS, LANES), jnp.float32)
            if not first:
                squares = norm_squares[rows, :]
            for lane in range(cols // LANES):
                here = slice(lane * LANES, (lane + 1) * LANES)
                values = read(rows, here).astype(jnp.float32)
                squares = squares + values * values
                xg[rows, at + here.start : at + here.stop] = (values * gains[:, here]).astype(
                    jnp.bfloat16
                )
            norm_squares[rows, :] = squares

    def project(layer, first_col, cols, span, first):
        rows = slice(*span)
        for half in range(2):
            held = slice(half * chans, (half + 1) * chans)
            product = dot_nt(xg[rows, :cols], wp[layer, half, :, pl.ds(first_col, cols)])
            if first:
                accp[rows, held] = product
            else:
                accp[rows, held] += product

    pending = []

    def remote(source, target, send, recv, device):
        copy = pltpu.make_async_remote_copy(
            src_ref=source,
            dst_ref=target,
            send_sem=send,
            recv_sem=recv,
            device_id=tp_id(device),
            device_id_type=MESH,
        )
        return copy

    def y_copy(phase, buf, step, chunk, owner, rows):
        target = lax.rem(my_y + step, n_y) * CORES + core
        ref = buf.at[owner, chunk, rows]
        return remote(
            ref, ref, y_send.at[phase, step, chunk], y_recv.at[phase, step, chunk], target
        )

    def f_copy(phase, buf, step, chunk, owner, rows):
        ref = buf.at[owner, chunk, rows]
        return remote(
            ref, ref, f_send.at[phase, step, chunk], f_recv.at[phase, step, chunk], sibling
        )

    def send_own(phase, buf, chunk, span):
        rows = pl.ds(span[0], span[1] - span[0])
        for step in range(1, n_y):
            copy = y_copy(phase, buf, step, chunk, me, rows)
            copy.start()
            pending.append(copy)
        copy = f_copy(phase, buf, 0, chunk, me, rows)
        copy.start()
        pending.append(copy)

    def near(phase, buf, chunks, span, use):
        rows = pl.ds(span[0], span[1] - span[0])
        use(me, range(chunks), span, True)
        for chunk in range(chunks):
            f_copy(phase, buf, 0, chunk, sibling, rows).wait_recv()
        use(sibling, range(chunks), span, False)

    def arrive(phase, buf, chunk, span, use):
        rows = pl.ds(span[0], span[1] - span[0])
        for step in range(1, n_y):
            owner = lax.rem(my_y + n_y - step, n_y) * CORES + core
            y_copy(phase, buf, step, chunk, owner, rows).wait_recv()
            copy = f_copy(phase, buf, step, chunk, owner, rows)
            copy.start()
            pending.append(copy)
            use(owner, (chunk,), span, False)

    def relayed(phase, buf, chunk, span, use):
        rows = pl.ds(span[0], span[1] - span[0])
        for step in range(1, n_y):
            owner = lax.rem(my_y + n_y - step, n_y) * CORES + 1 - core
            f_copy(phase, buf, step, chunk, owner, rows).wait_recv()
            use(owner, (chunk,), span, False)

    def far(phase, buf, chunks, span, use):
        for chunk in chunks:
            arrive(phase, buf, chunk, span, use)
            if chunk > 0:
                relayed(phase, buf, chunk - 1, span, use)

    def gate(first_row, count):
        rows = pl.ds(first_row, count)
        scaling = lax.rsqrt(
            jnp.sum(norm_squares[rows, :], axis=1, keepdims=True) / width + epsilon
        )
        value = accp[rows, :chans] * scaling
        gates = accp[rows, chans:] * scaling
        gated = (value * jax.nn.sigmoid(gates)).astype(jnp.bfloat16)
        widened = gated.astype(jnp.float32)
        for lane in range(chans // LANES):
            ext[lane, pl.ds(first_row + HALO, count), :] = widened[
                :, lane * LANES : (lane + 1) * LANES
            ]
        return gated

    def gate_rows(start, stop):
        @pl.loop(0, (stop - start) // HALO)
        def _(block):
            gate(pl.multiple_of(start + block * HALO, HALO), HALO)

    def halo_copy(layer):
        return pltpu.make_async_remote_copy(
            src_ref=halo_out.at[layer],
            dst_ref=halo_in.at[layer],
            send_sem=halo_send.at[layer],
            recv_sem=halo_recv.at[layer],
            device_id={"sp": lax.rem(sp + 1, n_sp)},
            device_id_type=MESH,
        )

    def send_halo(layer):
        halo_out[layer] = gate(tokens - HALO, HALO)

        @pl.when(sp < n_sp - 1)
        def _():
            halo_copy(layer).start()

    def receive_halo(layer):
        @pl.when(sp > 0)
        def _():
            halo_copy(layer).wait_recv()
            for lane in range(chans // LANES):
                ext[lane, :HALO, :] = halo_in[
                    layer, :, lane * LANES : (lane + 1) * LANES
                ].astype(jnp.float32)

        @pl.when(sp == 0)
        def _():
            ext[:, :HALO, :] = jnp.zeros((chans // LANES, HALO, LANES), jnp.float32)

    def convolve(layer, half, start, stop):
        base = spans[layer][half][0]
        blocks = []
        while start < stop:
            count = min(ROWS, stop - start)
            blocks.append((start, count))
            start += count

        @pl.loop(0, chans // LANES)
        def _(lane):
            here = pl.ds(pl.multiple_of(lane * LANES, LANES), LANES)
            bias = bias_ref[layer : layer + 1, here]
            for first_row, count in blocks:
                rows = slice(first_row, first_row + count)
                total = jnp.broadcast_to(bias, (count, LANES))
                for tap in range(K):
                    begin = first_row + HALO - K + 1 + tap
                    window = ext[lane, begin : begin + count, :]
                    total = total + window * taps[layer, tap : tap + 1, here]
                filt[rows, here] = total
                inner = slice(first_row - base, first_row - base + count)
                part[half, 0, inner, :] += total
                part[half, 1, inner, :] += total * total

    def stat_copy(layer, half, step, owner, target):
        ref = stat.at[layer, half, owner]
        index = layer * 2 + half
        return remote(ref, ref, stat_send.at[index, step], stat_recv.at[index, step], target)

    def send_stats(layer, half):
        first_row = jnp.sum(jnp.transpose(part[half, 0]), axis=0, keepdims=True)
        square_row = jnp.sum(jnp.transpose(part[half, 1]), axis=0, keepdims=True)
        row_index = lax.broadcasted_iota(jnp.int32, (8, padded), 0)
        stat[layer, half, me] = jnp.where(row_index == 0, first_row, square_row)
        for step in range(1, n_tp):
            copy = stat_copy(layer, half, step, me, lax.rem(me + step, n_tp))
            copy.start()
            pending.append(copy)

    def activate(layer, half, phase):
        for step in range(1, n_tp):
            origin = lax.rem(me + n_tp - step, n_tp)
            stat_copy(layer, half, step, origin, origin).wait_recv()
        totals = jnp.sum(stat[layer, half], axis=0) / total_chans
        mean_row = totals[0:1]
        rstd_row = lax.rsqrt(totals[1:2] - mean_row * mean_row + epsilon)
        column[0] = jnp.transpose(jnp.broadcast_to(mean_row, (LANES, padded)))
        column[1] = jnp.transpose(jnp.broadcast_to(rstd_row, (LANES, padded)))
        start, stop = spans[layer][half]
        for chunk in range(chans // CHUNK):

            @pl.loop(0, (stop - start) // HALO)
            def _(block):
                inner = pl.ds(pl.multiple_of(block * HALO, HALO), HALO)
                rows = pl.ds(pl.multiple_of(start + block * HALO, HALO), HALO)
                for lane in range(CHUNK // LANES):
                    here = slice(chunk * CHUNK + lane * LANES, chunk * CHUNK + (lane + 1) * LANES)
                    values = (filt[rows, here] - column[0, inner, :]) * column[1, inner, :]
                    values = (
                        values * chan_gain_ref[layer : layer + 1, here]
                        + chan_bias_ref[layer : layer + 1, here]
                    )
                    ag[layer, me, chunk, rows, lane * LANES : (lane + 1) * LANES] = (
                        jax.nn.silu(values).astype(jnp.bfloat16)
                    )

            send_own(phase, ag.at[layer], chunk, (start, stop))

    def use_activated(layer):
        def use(owner, chunks, span, first):
            rows = slice(*span)
            total = res[rows, :] if first else acco[rows, :]
            for chunk in chunks:
                start = pl.multiple_of(owner * chans + chunk * CHUNK, LANES)
                total = total + dot_nt(
                    ag[layer, owner, chunk, rows, :], wo[layer, :, pl.ds(start, CHUNK)]
                )
            acco[rows, :] = total

        return use

    def use_stream(owner, chunks, span, first):
        start = pl.multiple_of(owner * feats + chunks[0] * CHUNK, LANES)
        for chunk in chunks:
            prepare(
                1,
                lambda rows, here: sg[owner, chunk, rows, here],
                pl.multiple_of(owner * feats + chunk * CHUNK, LANES),
                CHUNK,
                span,
                (chunk - chunks[0]) * CHUNK,
                first and chunk == 0,
            )
        project(1, start, len(chunks) * CHUNK, span, first)

    n_a, n_f = chans // CHUNK, feats // CHUNK
    part[...] = jnp.zeros(part.shape, jnp.float32)
    for index in range(WEIGHT_PIECES):
        start = index * piece
        prepare(
            0,
            lambda rows, here: x_ref[rows, start + here.start : start + here.stop],
            start,
            piece,
            (0, tokens),
            0,
            index == 0,
        )
        for copy in proj_copies(0, index):
            copy.wait()
        project(0, start, piece, (0, tokens), index == 0)
    res[...] = x_ref[:, pl.ds(pl.multiple_of(me * feats, LANES), feats)].astype(jnp.float32)
    pl.semaphore_wait(
        barrier,
        n_tp - 1 + jnp.where(sp > 0, 1, 0) + jnp.where(sp < n_sp - 1, 1, 0),
    )
    late, early = spans[0]
    send_halo(0)
    gate_rows(0, tokens - HALO)
    convolve(0, 0, *late)
    send_stats(0, 0)
    convolve(0, 1, ROWS, early[1])
    receive_halo(0)
    convolve(0, 1, 0, ROWS)
    send_stats(0, 1)
    activate(0, 0, 0)
    activate(0, 1, 1)
    out_copy(0).wait()
    def send_stream(half, span):
        rows = slice(*span)
        for chunk in range(n_f):
            here = slice(chunk * CHUNK, (chunk + 1) * CHUNK)
            rounded = acco[rows, here].astype(jnp.bfloat16)
            sg[me, chunk, rows, :] = rounded
            send_own(2 + half, sg, chunk, span)
            res[rows, here] = rounded.astype(jnp.float32)

    use = use_activated(0)
    near(0, ag.at[0], n_a, late, use)
    far(0, ag.at[0], range(n_a), late, use)
    near(1, ag.at[0], n_a, early, use)
    relayed(0, ag.at[0], n_a - 1, late, use)
    send_stream(0, late)
    far(1, ag.at[0], range(n_a), early, use)
    part[...] = jnp.zeros(part.shape, jnp.float32)
    for index in range(WEIGHT_PIECES):
        for copy in proj_copies(1, index):
            copy.wait()
    near(2, sg, n_f, late, use_stream)
    relayed(1, ag.at[0], n_a - 1, early, use)
    send_stream(1, early)
    far(2, sg, range(n_f), late, use_stream)
    near(3, sg, n_f, early, use_stream)
    relayed(2, sg, n_f - 1, late, use_stream)
    send_halo(1)
    gate_rows(split, tokens - HALO)
    convolve(1, 0, *spans[1][0])
    send_stats(1, 0)
    far(3, sg, range(n_f // 2), early, use_stream)
    activate(1, 0, 4)
    far(3, sg, range(n_f // 2, n_f), early, use_stream)
    relayed(3, sg, n_f - 1, early, use_stream)
    gate_rows(0, split)
    convolve(1, 1, HALO, spans[1][1][1])
    receive_halo(1)
    convolve(1, 1, 0, HALO)
    send_stats(1, 1)
    out_copy(1).wait()
    use = use_activated(1)
    near(4, ag.at[1], n_a, spans[1][0], use)
    activate(1, 1, 5)
    far(4, ag.at[1], range(n_a), spans[1][0], use)
    near(5, ag.at[1], n_a, spans[1][1], use)
    relayed(4, ag.at[1], n_a - 1, spans[1][0], use)
    far(5, ag.at[1], range(n_a), spans[1][1], use)
    relayed(5, ag.at[1], n_a - 1, spans[1][1], use)
    out_ref[...] = acco[...].astype(jnp.bfloat16)

    @pl.when(sp < n_sp - 1)
    def _():
        for layer in range(LAYERS):
            halo_copy(layer).wait_send()

    for copy in pending:
        copy.wait_send()


def fused(mesh, stream, norm_gain, value_weight, gate_weight, conv_kernel, conv_bias,
          channel_gain, channel_bias, out_weight):
    n_tp, n_sp = mesh.shape["tp"], mesh.shape["sp"]
    width, tokens = stream.shape
    chans, feats = value_weight.shape[1], out_weight.shape[1]
    fits = (
        n_tp % CORES == 0
        and chans % CHUNK == 0
        and feats % CHUNK == 0
        and width % (WEIGHT_PIECES * CHUNK) == 0
        and tokens % ROWS == 0
        and (tokens // 2 - HALO) // HALO * HALO % ROWS == 0
        and tokens >= 4 * ROWS
        and LAYERS == 2
        and n_tp <= 8
    )
    if not fits:
        return local(stream, norm_gain, value_weight, gate_weight, conv_kernel, conv_bias,
                     channel_gain, channel_bias, out_weight)
    split = (tokens // 2 - HALO) // HALO * HALO
    padded = -(-(tokens - split) // LANES) * LANES
    n_y = n_tp // CORES
    n_a, n_f = chans // CHUNK, feats // CHUNK
    most = max(n_a, n_f)
    f32, bf16 = jnp.float32, jnp.bfloat16
    vmem = pl.BlockSpec(memory_space=pltpu.VMEM)
    anyspace = pl.BlockSpec(memory_space=pl.ANY)
    out = pl.pallas_call(
        functools.partial(kernel, n_tp, n_sp),
        out_shape=jax.ShapeDtypeStruct((tokens, feats), bf16),
        in_specs=[vmem] * 6 + [anyspace, anyspace, anyspace],
        out_specs=vmem,
        scratch_shapes=[
            pltpu.VMEM((LAYERS, 2, chans, width), bf16),
            pltpu.VMEM((LAYERS, feats, chans * n_tp), bf16),
            pltpu.VMEM((tokens, max(width // WEIGHT_PIECES, feats)), bf16),
            pltpu.VMEM((chans // LANES, HALO + tokens, LANES), f32),
            pltpu.VMEM((tokens, chans), f32),
            pltpu.VMEM((LAYERS, K, chans), f32),
            pltpu.VMEM((tokens, LANES), f32),
            pltpu.VMEM((2, 2, padded, LANES), f32),
            pltpu.VMEM((2, padded, LANES), f32),
            pltpu.VMEM((LAYERS, HALO, chans), bf16),
            pltpu.VMEM((LAYERS, HALO, chans), bf16),
            pltpu.VMEM((LAYERS, 2, n_tp, 8, padded), f32),
            pltpu.VMEM((LAYERS, n_tp, n_a, tokens, CHUNK), bf16),
            pltpu.VMEM((n_tp, n_f, tokens, CHUNK), bf16),
            pltpu.VMEM((tokens, 2 * chans), f32),
            pltpu.VMEM((tokens, feats), f32),
            pltpu.VMEM((tokens, feats), f32),
            pltpu.SemaphoreType.DMA((LAYERS, WEIGHT_PIECES)),
            pltpu.SemaphoreType.DMA((LAYERS,)),
            pltpu.SemaphoreType.DMA((LAYERS,)),
            pltpu.SemaphoreType.DMA((LAYERS,)),
            pltpu.SemaphoreType.DMA((LAYERS * 2, n_tp)),
            pltpu.SemaphoreType.DMA((LAYERS * 2, n_tp)),
            pltpu.SemaphoreType.DMA((6, n_y, most)),
            pltpu.SemaphoreType.DMA((6, n_y, most)),
            pltpu.SemaphoreType.DMA((6, n_y, most)),
            pltpu.SemaphoreType.DMA((6, n_y, most)),
        ],
        compiler_params=pltpu.CompilerParams(
            collective_id=0, has_side_effects=True, vmem_limit_bytes=60 * 1024 * 1024
        ),
    )(stream.T, norm_gain, jnp.transpose(conv_kernel, (2, 0, 1)), conv_bias, channel_gain, channel_bias,
       value_weight, gate_weight, out_weight)
    return out.T


def solution(mesh):
    placed = (
        P(None, ("grp", "sp")),
        P(),
        P(None, "tp", None),
        P(None, "tp", None),
        P(None, "tp", None),
        P(None, "tp"),
        P(None, "tp"),
        P(None, "tp"),
        P(None, "tp", None),
    )
    return jax.shard_map(
        functools.partial(fused, mesh), mesh=mesh, in_specs=placed, out_specs=P("tp", ("grp", "sp")), check_vma=False
    )
```

```python
import functools

import jax
import jax.numpy as jnp
from jax import lax
from jax.experimental import pallas as pl
from jax.experimental.pallas import tpu as pltpu
from jax.sharding import PartitionSpec as P

K = 31
LAYERS = 2


epsilon = 1e-06


def shifted(value, axis, steps):
    count = lax.axis_size(axis)
    initial, last = (max(0, -steps), min(count, count - steps))
    return lax.ppermute(value, axis, [(source, source + steps) for source in range(initial, last)])


def depthwise(signal, kernel):
    out = lax.conv_general_dilated(
        signal[None],
        kernel[:, None, :],
        (1,),
        [(0, 0)],
        dimension_numbers=("NCW", "OIW", "NCW"),
        feature_group_count=kernel.shape[0],
        precision=lax.Precision.HIGHEST,
    )
    return out[0]


def norm_project(whole, gain, weights):
    scaling = lax.rsqrt(jnp.mean(whole * whole, axis=0, keepdims=True) + epsilon)
    normed = (whole * scaling * gain[:, None]).astype(jnp.bfloat16)
    return jnp.dot(weights, normed, preferred_element_type=jnp.float32)


def local(
    stream,
    norm_gain,
    value_weight,
    gate_weight,
    conv_kernel,
    conv_bias,
    channel_gain,
    channel_bias,
    out_weight,
):
    shard_channels = value_weight.shape[1]
    total_channels = shard_channels * lax.axis_size("tp")
    shard_features = out_weight.shape[1]
    tokens_here = stream.shape[1]
    row_start = lax.axis_index("tp") * shard_features
    whole = stream.astype(jnp.float32)
    current = lax.dynamic_slice_in_dim(whole, row_start, shard_features, 0)
    layer_out = stream
    for layer in range(LAYERS):
        both_weights = jnp.concatenate((value_weight[layer], gate_weight[layer]), axis=0)
        if layer == 0:
            projected = norm_project(whole, norm_gain[layer], both_weights)
        else:
            gathered = lax.all_gather(layer_out, "tp", axis=0, tiled=True).astype(jnp.float32)
            projected = norm_project(gathered, norm_gain[layer], both_weights)
        gated = (projected[:shard_channels] * jax.nn.sigmoid(projected[shard_channels:])).astype(
            jnp.bfloat16
        )
        earlier = shifted(gated[:, tokens_here - (K - 1) :], "sp", 1)
        extended = jnp.concatenate((earlier, gated), axis=1).astype(jnp.float32)
        filtered = depthwise(extended, conv_kernel[layer]) + conv_bias[layer][:, None]
        first_sum, square_sum = lax.psum(
            (
                jnp.sum(filtered, axis=0, keepdims=True),
                jnp.sum(filtered * filtered, axis=0, keepdims=True),
            ),
            "tp",
        )
        row_mean = first_sum / total_channels
        centred = filtered - row_mean
        spread = square_sum / total_channels - row_mean * row_mean
        activated = jax.nn.silu(
            centred * lax.rsqrt(spread + epsilon) * channel_gain[layer][:, None]
            + channel_bias[layer][:, None]
        ).astype(jnp.bfloat16)

        def accumulate(total, piece, start, weights=out_weight[layer]):
            weight_cols = lax.dynamic_slice_in_dim(weights, start, piece.shape[0], 1)
            return total + jnp.dot(weight_cols, piece, preferred_element_type=jnp.float32)

        zero_branch = jnp.zeros((shard_features, tokens_here), jnp.float32)
        branch = accumulate(
            zero_branch, lax.all_gather(activated, "tp", axis=0, tiled=True), jnp.int32(0)
        )
        layer_out = (current + branch).astype(jnp.bfloat16)
        current = layer_out.astype(jnp.float32)
    return layer_out


MESH = pl.DeviceIdType.MESH
LANES = 128
CHUNK = 256
HALO = 32
ROWS = 64
CORES = 2
WEIGHT_PIECES = 4


def dot_nt(left, right):
    return lax.dot_general(
        left, right, (((1,), (1,)), ((), ())), preferred_element_type=jnp.float32
    )


def kernel(
    n_tp,
    n_sp,
    x_ref,
    gain_ref,
    taps_ref,
    bias_ref,
    chan_gain_ref,
    chan_bias_ref,
    wv_ref,
    wg_ref,
    ow_ref,
    out_ref,
    wp,
    wo,
    xg,
    ext,
    filt,
    taps,
    norm_squares,
    part,
    column,
    halo_out,
    halo_in,
    stat,
    ag,
    sg,
    accp,
    acco,
    res,
    wp_sem,
    wo_sem,
    halo_send,
    halo_recv,
    stat_send,
    stat_recv,
    y_send,
    y_recv,
    f_send,
    f_recv,
):
    tokens, width = x_ref.shape
    chans = wv_ref.shape[1]
    feats = ow_ref.shape[1]
    total_chans = chans * n_tp
    n_y = n_tp // CORES
    piece = width // WEIGHT_PIECES
    padded = part.shape[2]
    split = (tokens // 2 - HALO) // HALO * HALO
    spans = (
        ((split, tokens), (0, split)),
        ((split + HALO, tokens), (0, split + HALO)),
    )
    me = lax.axis_index("tp")
    sp = lax.axis_index("sp")
    my_y, core = me // CORES, me % CORES
    sibling = my_y * CORES + (1 - core)

    def tp_id(index):
        return {"tp": index}

    barrier = pltpu.get_barrier_semaphore()
    for step in range(1, n_tp):
        pl.semaphore_signal(
            barrier, inc=1, device_id=tp_id(lax.rem(me + step, n_tp)), device_id_type=MESH
        )

    @pl.when(sp > 0)
    def _():
        pl.semaphore_signal(barrier, inc=1, device_id={"sp": sp - 1}, device_id_type=MESH)

    @pl.when(sp < n_sp - 1)
    def _():
        pl.semaphore_signal(barrier, inc=1, device_id={"sp": sp + 1}, device_id_type=MESH)

    def proj_copies(layer, index):
        cols = pl.ds(index * piece, piece)
        return [
            pltpu.make_async_copy(
                ref.at[layer, :, cols], wp.at[layer, half, :, cols], wp_sem.at[layer, index]
            )
            for half, ref in enumerate((wv_ref, wg_ref))
        ]

    def out_copy(layer):
        return pltpu.make_async_copy(ow_ref.at[layer], wo.at[layer], wo_sem.at[layer])

    for layer in range(LAYERS):
        for index in range(WEIGHT_PIECES):
            for copy in proj_copies(layer, index):
                copy.start()
        out_copy(layer).start()

    for layer in range(LAYERS):
        taps[layer] = taps_ref[:, layer, :]

    def prepare(layer, read, first_col, cols, span, at, first):
        gains = gain_ref[layer : layer + 1, pl.ds(first_col, cols)]

        @pl.loop(0, (span[1] - span[0]) // ROWS)
        def _(block):
            rows = pl.ds(pl.multiple_of(span[0] + block * ROWS, HALO), ROWS)
            squares = jnp.zeros((ROWS, LANES), jnp.float32)
            if not first:
                squares = norm_squares[rows, :]
            for lane in range(cols // LANES):
                here = slice(lane * LANES, (lane + 1) * LANES)
                values = read(rows, here).astype(jnp.float32)
                squares = squares + values * values
                xg[rows, at + here.start : at + here.stop] = (values * gains[:, here]).astype(
                    jnp.bfloat16
                )
            norm_squares[rows, :] = squares

    def project(layer, first_col, cols, span, first):
        rows = slice(*span)
        for half in range(2):
            held = slice(half * chans, (half + 1) * chans)
            product = dot_nt(xg[rows, :cols], wp[layer, half, :, pl.ds(first_col, cols)])
            if first:
                accp[rows, held] = product
            else:
                accp[rows, held] += product

    pending = []

    def remote(source, target, send, recv, device):
        copy = pltpu.make_async_remote_copy(
            src_ref=source,
            dst_ref=target,
            send_sem=send,
            recv_sem=recv,
            device_id=tp_id(device),
            device_id_type=MESH,
        )
        return copy

    def y_copy(phase, buf, step, chunk, owner, rows):
        target = lax.rem(my_y + step, n_y) * CORES + core
        ref = buf.at[owner, chunk, rows]
        return remote(
            ref, ref, y_send.at[phase, step, chunk], y_recv.at[phase, step, chunk], target
        )

    def f_copy(phase, buf, step, chunk, owner, rows):
        ref = buf.at[owner, chunk, rows]
        return remote(
            ref, ref, f_send.at[phase, step, chunk], f_recv.at[phase, step, chunk], sibling
        )

    def send_own(phase, buf, chunk, span):
        rows = pl.ds(span[0], span[1] - span[0])
        for step in range(1, n_y):
            copy = y_copy(phase, buf, step, chunk, me, rows)
            copy.start()
            pending.append(copy)
        copy = f_copy(phase, buf, 0, chunk, me, rows)
        copy.start()
        pending.append(copy)

    def near(phase, buf, chunks, span, use):
        rows = pl.ds(span[0], span[1] - span[0])
        use(me, range(chunks), span, True)
        for chunk in range(chunks):
            f_copy(phase, buf, 0, chunk, sibling, rows).wait_recv()
        use(sibling, range(chunks), span, False)

    def arrive(phase, buf, chunk, span, use):
        rows = pl.ds(span[0], span[1] - span[0])
        for step in range(1, n_y):
            owner = lax.rem(my_y + n_y - step, n_y) * CORES + core
            y_copy(phase, buf, step, chunk, owner, rows).wait_recv()
            copy = f_copy(phase, buf, step, chunk, owner, rows)
            copy.start()
            pending.append(copy)
            use(owner, (chunk,), span, False)

    def relayed(phase, buf, chunk, span, use):
        rows = pl.ds(span[0], span[1] - span[0])
        for step in range(1, n_y):
            owner = lax.rem(my_y + n_y - step, n_y) * CORES + 1 - core
            f_copy(phase, buf, step, chunk, owner, rows).wait_recv()
            use(owner, (chunk,), span, False)

    def far(phase, buf, chunks, span, use):
        for chunk in chunks:
            arrive(phase, buf, chunk, span, use)
            if chunk > 0:
                relayed(phase, buf, chunk - 1, span, use)

    def gate(first_row, count):
        rows = pl.ds(first_row, count)
        scaling = lax.rsqrt(
            jnp.sum(norm_squares[rows, :], axis=1, keepdims=True) / width + epsilon
        )
        value = accp[rows, :chans] * scaling
        gates = accp[rows, chans:] * scaling
        gated = (value * jax.nn.sigmoid(gates)).astype(jnp.bfloat16)
        widened = gated.astype(jnp.float32)
        for lane in range(chans // LANES):
            ext[lane, pl.ds(first_row + HALO, count), :] = widened[
                :, lane * LANES : (lane + 1) * LANES
            ]
        return gated

    def gate_rows(start, stop):
        @pl.loop(0, (stop - start) // HALO)
        def _(block):
            gate(pl.multiple_of(start + block * HALO, HALO), HALO)

    def halo_copy(layer):
        return pltpu.make_async_remote_copy(
            src_ref=halo_out.at[layer],
            dst_ref=halo_in.at[layer],
            send_sem=halo_send.at[layer],
            recv_sem=halo_recv.at[layer],
            device_id={"sp": lax.rem(sp + 1, n_sp)},
            device_id_type=MESH,
        )

    def send_halo(layer):
        halo_out[layer] = gate(tokens - HALO, HALO)

        @pl.when(sp < n_sp - 1)
        def _():
            halo_copy(layer).start()

    def receive_halo(layer):
        @pl.when(sp > 0)
        def _():
            halo_copy(layer).wait_recv()
            for lane in range(chans // LANES):
                ext[lane, :HALO, :] = halo_in[
                    layer, :, lane * LANES : (lane + 1) * LANES
                ].astype(jnp.float32)

        @pl.when(sp == 0)
        def _():
            ext[:, :HALO, :] = jnp.zeros((chans // LANES, HALO, LANES), jnp.float32)

    def convolve(layer, half, start, stop):
        base = spans[layer][half][0]
        blocks = []
        while start < stop:
            count = min(ROWS, stop - start)
            blocks.append((start, count))
            start += count

        @pl.loop(0, chans // LANES)
        def _(lane):
            here = pl.ds(pl.multiple_of(lane * LANES, LANES), LANES)
            bias = bias_ref[layer : layer + 1, here]
            for first_row, count in blocks:
                rows = slice(first_row, first_row + count)
                total = jnp.broadcast_to(bias, (count, LANES))
                for tap in range(K):
                    begin = first_row + HALO - K + 1 + tap
                    window = ext[lane, begin : begin + count, :]
                    total = total + window * taps[layer, tap : tap + 1, here]
                filt[rows, here] = total
                inner = slice(first_row - base, first_row - base + count)
                part[half, 0, inner, :] += total
                part[half, 1, inner, :] += total * total

    def stat_copy(layer, half, step, owner, target):
        ref = stat.at[layer, half, owner]
        index = layer * 2 + half
        return remote(ref, ref, stat_send.at[index, step], stat_recv.at[index, step], target)

    def send_stats(layer, half):
        first_row = jnp.sum(jnp.transpose(part[half, 0]), axis=0, keepdims=True)
        square_row = jnp.sum(jnp.transpose(part[half, 1]), axis=0, keepdims=True)
        row_index = lax.broadcasted_iota(jnp.int32, (8, padded), 0)
        stat[layer, half, me] = jnp.where(row_index == 0, first_row, square_row)
        for step in range(1, n_tp):
            copy = stat_copy(layer, half, step, me, lax.rem(me + step, n_tp))
            copy.start()
            pending.append(copy)

    def activate(layer, half, phase):
        for step in range(1, n_tp):
            origin = lax.rem(me + n_tp - step, n_tp)
            stat_copy(layer, half, step, origin, origin).wait_recv()
        totals = jnp.sum(stat[layer, half], axis=0) / total_chans
        mean_row = totals[0:1]
        rstd_row = lax.rsqrt(totals[1:2] - mean_row * mean_row + epsilon)
        column[0] = jnp.transpose(jnp.broadcast_to(mean_row, (LANES, padded)))
        column[1] = jnp.transpose(jnp.broadcast_to(rstd_row, (LANES, padded)))
        start, stop = spans[layer][half]
        for chunk in range(chans // CHUNK):

            @pl.loop(0, (stop - start) // HALO)
            def _(block):
                inner = pl.ds(pl.multiple_of(block * HALO, HALO), HALO)
                rows = pl.ds(pl.multiple_of(start + block * HALO, HALO), HALO)
                for lane in range(CHUNK // LANES):
                    here = slice(chunk * CHUNK + lane * LANES, chunk * CHUNK + (lane + 1) * LANES)
                    values = (filt[rows, here] - column[0, inner, :]) * column[1, inner, :]
                    values = (
                        values * chan_gain_ref[layer : layer + 1, here]
                        + chan_bias_ref[layer : layer + 1, here]
                    )
                    ag[layer, me, chunk, rows, lane * LANES : (lane + 1) * LANES] = (
                        jax.nn.silu(values).astype(jnp.bfloat16)
                    )

            send_own(phase, ag.at[layer], chunk, (start, stop))

    def use_activated(layer):
        def use(owner, chunks, span, first):
            rows = slice(*span)
            total = res[rows, :] if first else acco[rows, :]
            for chunk in chunks:
                start = pl.multiple_of(owner * chans + chunk * CHUNK, LANES)
                total = total + dot_nt(
                    ag[layer, owner, chunk, rows, :], wo[layer, :, pl.ds(start, CHUNK)]
                )
            acco[rows, :] = total

        return use

    def use_stream(owner, chunks, span, first):
        start = pl.multiple_of(owner * feats + chunks[0] * CHUNK, LANES)
        for chunk in chunks:
            prepare(
                1,
                lambda rows, here: sg[owner, chunk, rows, here],
                pl.multiple_of(owner * feats + chunk * CHUNK, LANES),
                CHUNK,
                span,
                (chunk - chunks[0]) * CHUNK,
                first and chunk == 0,
            )
        project(1, start, len(chunks) * CHUNK, span, first)

    n_a, n_f = chans // CHUNK, feats // CHUNK
    part[...] = jnp.zeros(part.shape, jnp.float32)
    for index in range(WEIGHT_PIECES):
        start = index * piece
        prepare(
            0,
            lambda rows, here: x_ref[rows, start + here.start : start + here.stop],
            start,
            piece,
            (0, tokens),
            0,
            index == 0,
        )
        for copy in proj_copies(0, index):
            copy.wait()
        project(0, start, piece, (0, tokens), index == 0)
    res[...] = x_ref[:, pl.ds(pl.multiple_of(me * feats, LANES), feats)].astype(jnp.float32)
    pl.semaphore_wait(
        barrier,
        n_tp - 1 + jnp.where(sp > 0, 1, 0) + jnp.where(sp < n_sp - 1, 1, 0),
    )
    late, early = spans[0]
    send_halo(0)
    gate_rows(0, tokens - HALO)
    convolve(0, 0, *late)
    send_stats(0, 0)
    convolve(0, 1, ROWS, early[1])
    receive_halo(0)
    convolve(0, 1, 0, ROWS)
    send_stats(0, 1)
    activate(0, 0, 0)
    activate(0, 1, 1)
    out_copy(0).wait()
    def send_stream(half, span):
        rows = slice(*span)
        for chunk in range(n_f):
            here = slice(chunk * CHUNK, (chunk + 1) * CHUNK)
            rounded = acco[rows, here].astype(jnp.bfloat16)
            sg[me, chunk, rows, :] = rounded
            send_own(2 + half, sg, chunk, span)
            res[rows, here] = rounded.astype(jnp.float32)

    use = use_activated(0)
    near(0, ag.at[0], n_a, late, use)
    far(0, ag.at[0], range(n_a), late, use)
    near(1, ag.at[0], n_a, early, use)
    relayed(0, ag.at[0], n_a - 1, late, use)
    send_stream(0, late)
    far(1, ag.at[0], range(n_a), early, use)
    part[...] = jnp.zeros(part.shape, jnp.float32)
    for index in range(WEIGHT_PIECES):
        for copy in proj_copies(1, index):
            copy.wait()
    near(2, sg, n_f, late, use_stream)
    relayed(1, ag.at[0], n_a - 1, early, use)
    send_stream(1, early)
    far(2, sg, range(n_f), late, use_stream)
    near(3, sg, n_f, early, use_stream)
    relayed(2, sg, n_f - 1, late, use_stream)
    send_halo(1)
    gate_rows(split, tokens - HALO)
    convolve(1, 0, *spans[1][0])
    send_stats(1, 0)
    far(3, sg, range(n_f // 2), early, use_stream)
    activate(1, 0, 4)
    far(3, sg, range(n_f // 2, n_f), early, use_stream)
    relayed(3, sg, n_f - 1, early, use_stream)
    gate_rows(0, split)
    convolve(1, 1, HALO, spans[1][1][1])
    receive_halo(1)
    convolve(1, 1, 0, HALO)
    send_stats(1, 1)
    out_copy(1).wait()
    use = use_activated(1)
    near(4, ag.at[1], n_a, spans[1][0], use)
    activate(1, 1, 5)
    far(4, ag.at[1], range(n_a), spans[1][0], use)
    near(5, ag.at[1], n_a, spans[1][1], use)
    relayed(4, ag.at[1], n_a - 1, spans[1][0], use)
    far(5, ag.at[1], range(n_a), spans[1][1], use)
    relayed(5, ag.at[1], n_a - 1, spans[1][1], use)
    out_ref[...] = acco[...].astype(jnp.bfloat16)

    @pl.when(sp < n_sp - 1)
    def _():
        for layer in range(LAYERS):
            halo_copy(layer).wait_send()

    for copy in pending:
        copy.wait_send()


def hand_over(from_ref, to_ref):
    to_ref[...] = from_ref[...]


def fused(mesh, stream, norm_gain, value_weight, gate_weight, conv_kernel, conv_bias,
          channel_gain, channel_bias, out_weight):
    n_tp, n_sp = mesh.shape["tp"], mesh.shape["sp"]
    width, tokens = stream.shape
    chans, feats = value_weight.shape[1], out_weight.shape[1]
    fits = (
        n_tp % CORES == 0
        and chans % CHUNK == 0
        and feats % CHUNK == 0
        and width % (WEIGHT_PIECES * CHUNK) == 0
        and tokens % ROWS == 0
        and (tokens // 2 - HALO) // HALO * HALO % ROWS == 0
        and tokens >= 4 * ROWS
        and LAYERS == 2
        and n_tp <= 8
    )
    if not fits:
        return local(stream, norm_gain, value_weight, gate_weight, conv_kernel, conv_bias,
                     channel_gain, channel_bias, out_weight)
    split = (tokens // 2 - HALO) // HALO * HALO
    padded = -(-(tokens - split) // LANES) * LANES
    n_y = n_tp // CORES
    n_a, n_f = chans // CHUNK, feats // CHUNK
    most = max(n_a, n_f)
    f32, bf16 = jnp.float32, jnp.bfloat16
    vmem = pl.BlockSpec(memory_space=pltpu.VMEM)
    anyspace = pl.BlockSpec(memory_space=pl.ANY)
    out = pl.pallas_call(
        functools.partial(kernel, n_tp, n_sp),
        out_shape=jax.ShapeDtypeStruct((tokens, feats), bf16),
        in_specs=[vmem] * 6 + [anyspace, anyspace, anyspace],
        out_specs=vmem,
        scratch_shapes=[
            pltpu.VMEM((LAYERS, 2, chans, width), bf16),
            pltpu.VMEM((LAYERS, feats, chans * n_tp), bf16),
            pltpu.VMEM((tokens, max(width // WEIGHT_PIECES, feats)), bf16),
            pltpu.VMEM((chans // LANES, HALO + tokens, LANES), f32),
            pltpu.VMEM((tokens, chans), f32),
            pltpu.VMEM((LAYERS, K, chans), f32),
            pltpu.VMEM((tokens, LANES), f32),
            pltpu.VMEM((2, 2, padded, LANES), f32),
            pltpu.VMEM((2, padded, LANES), f32),
            pltpu.VMEM((LAYERS, HALO, chans), bf16),
            pltpu.VMEM((LAYERS, HALO, chans), bf16),
            pltpu.VMEM((LAYERS, 2, n_tp, 8, padded), f32),
            pltpu.VMEM((LAYERS, n_tp, n_a, tokens, CHUNK), bf16),
            pltpu.VMEM((n_tp, n_f, tokens, CHUNK), bf16),
            pltpu.VMEM((tokens, 2 * chans), f32),
            pltpu.VMEM((tokens, feats), f32),
            pltpu.VMEM((tokens, feats), f32),
            pltpu.SemaphoreType.DMA((LAYERS, WEIGHT_PIECES)),
            pltpu.SemaphoreType.DMA((LAYERS,)),
            pltpu.SemaphoreType.DMA((LAYERS,)),
            pltpu.SemaphoreType.DMA((LAYERS,)),
            pltpu.SemaphoreType.DMA((LAYERS * 2, n_tp)),
            pltpu.SemaphoreType.DMA((LAYERS * 2, n_tp)),
            pltpu.SemaphoreType.DMA((6, n_y, most)),
            pltpu.SemaphoreType.DMA((6, n_y, most)),
            pltpu.SemaphoreType.DMA((6, n_y, most)),
            pltpu.SemaphoreType.DMA((6, n_y, most)),
        ],
        compiler_params=pltpu.CompilerParams(
            collective_id=0, has_side_effects=True, vmem_limit_bytes=60 * 1024 * 1024
        ),
    )(stream.T, norm_gain, jnp.transpose(conv_kernel, (2, 0, 1)), conv_bias, channel_gain, channel_bias,
       value_weight, gate_weight, out_weight)
    out = pl.pallas_call(
        hand_over,
        out_shape=jax.ShapeDtypeStruct(out.shape, out.dtype),
        in_specs=[vmem],
        out_specs=vmem,
    )(out)
    return out.T


def solution(mesh):
    placed = (
        P(None, ("grp", "sp")),
        P(),
        P(None, "tp", None),
        P(None, "tp", None),
        P(None, "tp", None),
        P(None, "tp"),
        P(None, "tp"),
        P(None, "tp"),
        P(None, "tp", None),
    )
    return jax.shard_map(
        functools.partial(fused, mesh), mesh=mesh, in_specs=placed, out_specs=P("tp", ("grp", "sp")), check_vma=False
    )
```
